128 devices in a mesh: kv: 32 (over z, y, core), tp: 4 (over x).
Axes of the slice: x: 4, y: 4, z: 4, core: 2. Of those that a mesh axis runs over, the one named last changes fastest.
Arguments:
- tokens: bfloat16 [512, 4, 4096], P('kv'), may hold values from -6 to 6
- norm_gain: bfloat16 [4096], replicated, may hold values from 0.099609375 to 1.8984375
- query_weight: bfloat16 [4096, 2048], P(None, 'tp'), may hold values from -0.09375 to 0.09375
- key_weight: bfloat16 [4096, 2048], P(None, 'tp'), may hold values from -0.09375 to 0.09375
- value_weight: bfloat16 [4096, 2048], P(None, 'tp'), may hold values from -0.09375 to 0.09375
- outgate_weight: bfloat16 [4096, 2048], P(None, 'tp'), may hold values from -0.09375 to 0.09375
- gate_weight: bfloat16 [4096, 32], replicated, may hold values from -0.09375 to 0.09375
- gate_bias: float32 [2, 16], replicated, may hold values from -1 to 4
- head_gain: bfloat16 [2048], P('tp'), may hold values from 0.099609375 to 1.8984375
- out_weight: bfloat16 [2048, 4096], P('tp', 'kv'), may hold values from -0.125 to 0.125
- state_c: float32 [512, 16, 128, 128], P('kv', 'tp'), may hold values from -3 to 3
- state_n: float32 [512, 16, 128], P('kv', 'tp'), may hold values from -3 to 3
- state_m: float32 [512, 16], P('kv', 'tp'), may hold values from -1 to 2
- prev_keys: bfloat16 [512, 16, 4, 128], P('kv', 'tp'), may hold values from -6 to 6
- prev_values: bfloat16 [512, 16, 4, 128], P('kv', 'tp'), may hold values from -6 to 6
- prev_gates: float32 [512, 16, 2, 4], P('kv', 'tp'), may hold values from -2 to 5
- accepted: int32 [512], P('kv'), may hold values from 0 to 4
Outputs:
- mixed: bfloat16 [512, 4, 4096], P(None, None, 'kv')
- carried_c: float32 [512, 16, 128, 128], P('kv', 'tp')
- carried_n: float32 [512, 16, 128], P('kv', 'tp')
- carried_m: float32 [512, 16], P('kv', 'tp')
- step_keys: bfloat16 [512, 16, 4, 128], P('kv', 'tp')
- step_values: bfloat16 [512, 16, 4, 128], P('kv', 'tp')
- step_gates: float32 [512, 16, 2, 4], P('kv', 'tp')
The draws below stay inside these ranges and needn't reach their ends.
Inputs may be any that keep to these rules, and one draw needn't show every extreme that they name: accepted counts proposals of the last step, from none to all 4.
All inputs are finite; a program needn't handle non-finite values.
Results may differ from the reference program's by a relative error of at most 0.0075.
The reference program's roundings to bfloat16 on the way (of `normed`, `queries`, `outgate` and `gated`) count: a program that leaves them out, or rounds other values in their place, can miss the bound.
Values may be sent and summed in bfloat16 or wider, within the bound.
A program may use at most 128 MiB of HBM per device.

```python
import jax
import jax.numpy as jnp
from jax import lax

D = 4096
HEADS = 16
DH = 128
PROPS = 4
BATCH = 512
MIX = 2048


def touch_ends(values, rng, smallest, top_value):
    spot = [jax.random.randint(jax.random.fold_in(rng, axis), (), 0, length) for axis, length in enumerate(values.shape)]
    main_axis = values.shape.index(max(values.shape))
    neighbour = spot[:main_axis] + [(spot[main_axis] + 1) % values.shape[main_axis]] + spot[main_axis + 1:]
    return values.at[tuple(spot)].set(smallest).at[tuple(neighbour)].set(top_value)


def level_of(stream_key, dims, split, low, largest):
    loudness, own = 1.0, jax.random.fold_in(stream_key, 6)
    for axis_at, parts in split:
        draws = jnp.exp(jax.random.uniform(jax.random.fold_in(own, axis_at), (parts,), jnp.float32, low / len(split), largest / len(split)))
        loudness = loudness * jnp.repeat(draws, dims[axis_at] // parts).reshape([-1 if axis == axis_at else 1 for axis in range(len(dims))])
    return loudness


def normal_values(rng, extent, width, most, pieces=(), kind=jnp.bfloat16):
    values = jax.random.normal(rng, extent, jnp.float32) * width
    if len(pieces) > 0:
        values = level_of(rng, extent, pieces, -0.22, 0.18) * values
    return jnp.clip(values, min=-most, max=most).astype(kind)


def setup_inputs(seed: int = 0) -> dict:
    streams_of = jax.random.split(jax.random.key(seed), 18)
    tokens = normal_values(streams_of[0], (BATCH, PROPS, D), 1.0, 6.0, ((0, 32),))
    norm_gain = jnp.clip(1.0 + 0.18 * jax.random.normal(streams_of[1], (D,), jnp.float32), 0.099609375, 1.8984375).astype(jnp.bfloat16)
    query_weight = normal_values(streams_of[2], (D, MIX), D ** -0.5, 0.09375, ((1, 4),))
    key_weight = normal_values(streams_of[3], (D, MIX), D ** -0.5, 0.09375, ((1, 4),))
    value_weight = normal_values(streams_of[4], (D, MIX), D ** -0.5, 0.09375, ((1, 4),))
    outgate_weight = normal_values(streams_of[5], (D, MIX), D ** -0.5, 0.09375, ((1, 4),))
    gate_weight = normal_values(streams_of[6], (D, 2 * HEADS), D ** -0.5, 0.09375)
    gate_bias = jnp.clip(jax.random.uniform(streams_of[7], (2, HEADS), jnp.float32, -1.0, 4.0), -1.0, 4.0)
    head_gain = jnp.clip(1.0 + 0.18 * jax.random.normal(streams_of[8], (MIX,), jnp.float32), 0.099609375, 1.8984375).astype(jnp.bfloat16)
    out_weight = normal_values(streams_of[9], (MIX, D), MIX ** -0.5, 0.125, ((0, 4), (1, 32)))
    state_c = normal_values(streams_of[10], (BATCH, HEADS, DH, DH), 0.3, 3.0, ((0, 32), (1, 4)), jnp.float32)
    state_n = normal_values(streams_of[11], (BATCH, HEADS, DH), 0.3, 3.0, ((0, 32), (1, 4)), jnp.float32)
    state_m = jnp.clip(-1.0 + 3.0 * jax.random.uniform(streams_of[12], (BATCH, HEADS), jnp.float32) ** level_of(streams_of[12], (BATCH, HEADS), ((0, 32), (1, 4)), -0.2, 0.2), -1.0, 2.0)
    prev_keys = normal_values(streams_of[13], (BATCH, HEADS, PROPS, DH), 1.0, 6.0, ((0, 32), (1, 4)))
    prev_values = normal_values(streams_of[14], (BATCH, HEADS, PROPS, DH), 1.0, 6.0, ((0, 32), (1, 4)))
    prev_gates = jnp.clip(-2.0 + 7.0 * jax.random.uniform(streams_of[15], (BATCH, HEADS, 2, PROPS), jnp.float32) ** level_of(streams_of[15], (BATCH, HEADS, 2, PROPS), ((0, 32), (1, 4)), -0.2, 0.2), -2.0, 5.0)
    accepted = touch_ends(jax.random.randint(streams_of[16], (BATCH,), 0, PROPS + 1), jax.random.fold_in(streams_of[16], 1), 0, PROPS).astype(jnp.int32)
    return {"tokens": tokens, "norm_gain": norm_gain, "query_weight": query_weight, "key_weight": key_weight, "value_weight": value_weight, "outgate_weight": outgate_weight, "gate_weight": gate_weight, "gate_bias": gate_bias, "head_gain": head_gain, "out_weight": out_weight, "state_c": state_c, "state_n": state_n, "state_m": state_m, "prev_keys": prev_keys, "prev_values": prev_values, "prev_gates": prev_gates, "accepted": accepted}


EPSILON = 1e-06
HIGHEST = lax.Precision.HIGHEST

def replay(state_c, state_n, state_m, keys_in, values_in, gates_in, accepted):
    proposals = keys_in.shape[2]
    scaled = keys_in.astype(jnp.float32) * keys_in.shape[3] ** (-0.5)
    values_f = values_in.astype(jnp.float32)
    igates = gates_in[:, :, 0, :]
    forget = jax.nn.log_sigmoid(gates_in[:, :, 1, :])
    position = jnp.arange(proposals, dtype=jnp.int32)
    within = position[None, None, :] < accepted.astype(jnp.int32)[:, None, None]
    masked = jnp.where(within, forget, 0.0)
    summed = lax.optimization_barrier(jnp.sum(masked, axis=-1))
    log_weight = jnp.where(within, summed[..., None] - jnp.cumsum(masked, axis=-1) + igates, -jnp.inf)
    carried_m = jnp.maximum(summed + state_m, lax.optimization_barrier(jnp.max(log_weight, axis=-1)))
    shrink = jnp.exp(summed + state_m - carried_m)
    weights = jnp.exp(log_weight - carried_m[..., None])
    carried_c = shrink[..., None, None] * state_c + jnp.einsum('bhs,bhsv,bhsd->bhvd', weights, values_f, scaled, precision=HIGHEST)
    carried_n = shrink[..., None] * state_n + jnp.einsum('bhs,bhsd->bhd', weights, scaled, precision=HIGHEST)
    return (carried_c, carried_n, carried_m)

def cell_block(state_c, state_n, state_m, queries, scaled, values_f, igates, forget):
    proposals = queries.shape[2]
    cumul = jnp.cumsum(forget, axis=-1)
    causal = jnp.tril(jnp.ones((proposals, proposals), dtype=bool))
    log_decay = jnp.where(causal, cumul[..., :, None] - cumul[..., None, :] + igates[..., None, :], -jnp.inf)
    carried = cumul + state_m[..., None]
    stable = jnp.maximum(carried, lax.optimization_barrier(jnp.max(log_decay, axis=-1)))
    scores = jnp.einsum('bhtd,bhsd->bhts', queries, scaled, precision=HIGHEST) * jnp.exp(log_decay - stable[..., None])
    weight_state = jnp.exp(carried - stable)
    numer = weight_state[..., None] * jnp.einsum('bhvd,bhtd->bhtv', state_c, queries, precision=HIGHEST)
    numer = numer + jnp.einsum('bhts,bhsv->bhtv', scores, values_f, precision=HIGHEST)
    denom = weight_state * jnp.einsum('bhd,bhtd->bht', state_n, queries, precision=HIGHEST) + lax.optimization_barrier(jnp.sum(scores, axis=-1))
    return numer / jnp.maximum(jnp.abs(denom), jnp.exp(-stable))[..., None]

def gate_heads(hidden, gain, outgate):
    heads_count = hidden.shape[1]
    head_size = hidden.shape[3]
    normed = hidden * lax.rsqrt(lax.optimization_barrier(jnp.mean(hidden * hidden, axis=-1, keepdims=True)) + EPSILON)
    normed = normed * gain.astype(jnp.float32).reshape(heads_count, head_size)[None, :, None, :]
    rows_out = jnp.transpose(normed, (0, 2, 1, 3)).reshape(outgate.shape)
    return (rows_out * jax.nn.sigmoid(outgate.astype(jnp.float32))).astype(jnp.bfloat16)

def reference(tokens, norm_gain, query_weight, key_weight, value_weight, outgate_weight, gate_weight, gate_bias, head_gain, out_weight, state_c, state_n, state_m, prev_keys, prev_values, prev_gates, accepted):
    batch_count = tokens.shape[0]
    tokens_f = tokens.astype(jnp.float32)
    normed = tokens_f * lax.rsqrt(lax.optimization_barrier(jnp.mean(tokens_f * tokens_f, axis=-1, keepdims=True)) + EPSILON)
    normed = (normed * norm_gain.astype(jnp.float32)).astype(jnp.bfloat16)
    rows_in = normed.reshape(batch_count * PROPS, D)

    def project(matrix):
        return jnp.dot(rows_in, matrix, preferred_element_type=jnp.float32).astype(jnp.bfloat16)

    def by_head(array):
        return array.reshape(batch_count, PROPS, HEADS, DH).transpose(0, 2, 1, 3)
    queries = project(query_weight)
    step_keys = by_head(project(key_weight))
    step_values = by_head(project(value_weight))
    outgate = project(outgate_weight)
    all_gates = jnp.dot(rows_in, gate_weight, preferred_element_type=jnp.float32) + gate_bias.reshape(-1)[None, :]
    igates = all_gates[:, :HEADS].reshape(batch_count, PROPS, HEADS).transpose(0, 2, 1)
    fgates = all_gates[:, HEADS:].reshape(batch_count, PROPS, HEADS).transpose(0, 2, 1)
    step_gates = jnp.stack([igates, fgates], axis=2)
    carried_c, carried_n, carried_m = replay(state_c, state_n, state_m, prev_keys, prev_values, prev_gates, accepted)
    hidden = cell_block(carried_c, carried_n, carried_m, by_head(queries).astype(jnp.float32), step_keys.astype(jnp.float32) * DH ** (-0.5), step_values.astype(jnp.float32), igates, jax.nn.log_sigmoid(fgates))
    gated = gate_heads(hidden, head_gain, outgate)
    mixed = jnp.dot(gated, out_weight, preferred_element_type=jnp.float32).astype(jnp.bfloat16)
    mixed = mixed.reshape(batch_count, PROPS, D)
    return (mixed, carried_c, carried_n, carried_m, step_keys, step_values, step_gates)
```

```python
import functools

import jax
import jax.numpy as jnp
from jax import lax
from jax.experimental import pallas as pl
from jax.experimental.pallas import tpu as pltpu
from jax.sharding import PartitionSpec as P

EPSILON = 1e-06
NEG = -1e30
F32 = jnp.float32
BF16 = jnp.bfloat16
NT = (((1,), (1,)), ((), ()))

SEQS = 16
PROPS = 4
HEADS = 4
DH = 128
D = 4096
ROWS = SEQS * PROPS
MIXL = HEADS * DH
KCHUNKS = 4
KC = D // KCHUNKS


def nt_dot(a, b):
    return lax.dot_general(a, b, NT, preferred_element_type=F32)


def split(x):
    hi = x.astype(BF16)
    return hi, (x - hi.astype(F32)).astype(BF16)


def log_sigmoid(x):
    return jnp.minimum(x, 0.0) - jnp.log1p(jnp.exp(-jnp.abs(x)))


def roll(x, shift, axis):
    return pltpu.roll(x, shift % x.shape[axis], axis)


def iota(shape, axis):
    return lax.broadcasted_iota(jnp.int32, shape, axis)


def cumsum4(x, s):
    x = x + jnp.where(s >= 1, roll(x, 1, 0), 0.0)
    return x + jnp.where(s >= 2, roll(x, 2, 0), 0.0)


def spread(packed, expand, ztile):
    rows = packed.shape[0]
    ztile[0:rows, :] = packed
    turned = ztile[...].T
    for s in range(PROPS):
        expand[pl.ds(s, SEQS, stride=PROPS), :] = turned[0:SEQS, :]
    wide = expand[...]
    own = jnp.where(iota(wide.shape, 1) % PROPS == iota(wide.shape, 0) % PROPS, wide, 0.0)
    return own + roll(own, -1, 1) + roll(own, -2, 1) + roll(own, -3, 1)


def front_kernel(
    tok, gain, wq, wk, wv, wo, gwt, bias, hgain, sc, sn, sm, pk, pv, pg, acc,
    gated, cc, cn, cm, sk, sv, sg,
    tok_v, gain_v, w_v, gwt_v, bias_s, hgain_v, c_v, sn_v, sm_v, pk_v, pv_v, pg_v, acc_v,
    x_v, nb_v, f1_v, kp_v, vp_v, gates_v, gt_v, lane_v, ztile, expand, turn_v, cn_v, cm_v, sk_v, sv_v, sg_v, gated_v,
    in_sem, w_sem, c_sem, co_sem, out_sem,
):
    tp = lax.axis_index("tp")
    small = [
        (pg, pg_v), (acc, acc_v), (sm, sm_v), (pk, pk_v), (pv, pv_v), (tok, tok_v), (gain, gain_v),
        (sn, sn_v), (bias, bias_s), (hgain, hgain_v), (gwt, gwt_v),
    ]
    copies = {}
    for n, (src, dst) in enumerate(small):
        copies[n] = pltpu.make_async_copy(src, dst, in_sem.at[n])
        copies[n].start()
    state_in = []
    for h in range(HEADS):
        state_in.append(pltpu.make_async_copy(sc.at[:, h], c_v.at[h], c_sem.at[h]))
        state_in[h].start()
    w_in = []
    for n, w in enumerate((wq, wk, wv, wo)):
        w_in.append([])
        for k in range(KCHUNKS):
            span = pl.ds(k * KC, KC)
            w_in[n].append(pltpu.make_async_copy(w.at[span], w_v.at[n, span], w_sem.at[n, k]))
            w_in[n][k].start()

    row = iota((8 * HEADS, 128), 0)
    s = row % PROPS
    igate_row = row % 8 < PROPS
    lane_v[...] = jnp.zeros_like(lane_v)
    ztile[...] = jnp.zeros_like(ztile)

    for n in range(3):
        copies[n].wait()
    lane_v[0 : 8 * HEADS, 0:SEQS] = pg_v[...]
    lane_v[32:33, 0:SEQS] = acc_v[...].astype(F32)
    lane_v[40:44, 0:SEQS] = sm_v[...]
    igates = lane_v[0 : 8 * HEADS, :]
    accepted = lane_v[32:33, :]
    state_m = jnp.concatenate(
        [jnp.broadcast_to(lane_v[40 + h : 41 + h, :], (8, 128)) for h in range(HEADS)], axis=0
    )
    within = (s.astype(F32) < accepted) & igate_row
    masked = jnp.where(within, log_sigmoid(roll(igates, -4, 0)), 0.0)
    cums = cumsum4(masked, s)
    summed = jnp.where((s == 3) & igate_row, cums, 0.0)
    summed = summed + roll(summed, -1, 0)
    summed = summed + roll(summed, -2, 0)
    log_weight = jnp.where(within, summed - cums + igates, NEG)
    top = jnp.maximum(log_weight, jnp.where(s % 2 == 0, roll(log_weight, -1, 0), roll(log_weight, 1, 0)))
    top = jnp.maximum(top, jnp.where(s < 2, roll(top, -2, 0), roll(top, 2, 0)))
    carried_m = jnp.maximum(summed + state_m, top)
    shrink = jnp.exp(summed + state_m - carried_m)
    weights = jnp.exp(log_weight - carried_m)
    for h in range(HEADS):
        cm_v[h : h + 1, :] = carried_m[8 * h : 8 * h + 1, 0:SEQS]
    cols = spread(jnp.where(igate_row, weights, roll(shrink, 4, 0)), expand, ztile)

    copies[3].wait()
    copies[4].wait()
    for src, dst in ((pk_v, kp_v), (pv_v, vp_v)):
        f1_v[...] = src[...].astype(F32)
        for h in range(HEADS):
            for p in range(PROPS):
                dst[h, pl.ds(p, SEQS, stride=PROPS), :] = f1_v[pl.ds(h * PROPS + p, SEQS, stride=SEQS), :]

    copies[5].wait()
    copies[6].wait()
    for b in range(SEQS):
        x_v[PROPS * b : PROPS * (b + 1), :] = tok_v[b].astype(F32)
    gain_f = gain_v[...].astype(F32)
    for r in range(0, ROWS, 16):
        x = x_v[r : r + 16, :]
        x = x * lax.rsqrt(jnp.mean(x * x, axis=-1, keepdims=True) + EPSILON)
        nb_v[r : r + 16, :] = (x * gain_f).astype(BF16)

    copies[7].wait()
    lane = iota((1, 128), 1)
    sub = iota((ROWS, 128), 0)
    lane_full = iota((ROWS, 128), 1)
    shrink_bh = jnp.sum(
        jnp.where(lane_full == 8 * (sub % HEADS) + 4, cols, 0.0), axis=-1, keepdims=True
    )
    carried_n = shrink_bh * sn_v[...]
    state_out = []
    for h in range(HEADS):
        wkeys = kp_v[h] * (DH ** -0.5) * cols[:, 8 * h : 8 * h + 1]
        total = wkeys + jnp.where(sub % 2 == 0, roll(wkeys, -1, 0), roll(wkeys, 1, 0))
        total = total + jnp.where(sub % 4 < 2, roll(total, -2, 0), roll(total, 2, 0))
        carried_n = carried_n + jnp.where(sub % HEADS == h, total, 0.0)
        rhs = jnp.concatenate(split(wkeys), axis=0)
        vp = vp_v[h]
        vt = jnp.concatenate([vp, vp], axis=0).T.astype(BF16)
        state_in[h].wait()
        for b0 in range(0, SEQS, 4):
            lhs = jnp.concatenate(
                [vt * ((lane % ROWS) // PROPS == b).astype(F32).astype(BF16) for b in range(b0, b0 + 4)], axis=0
            )
            update = jnp.dot(lhs, rhs, preferred_element_type=F32)
            for n in range(4):
                b = b0 + n
                c_v[h, b] = (
                    cols[PROPS * b : PROPS * b + 1, 8 * h + 4 : 8 * h + 5] * c_v[h, b]
                    + update[DH * n : DH * (n + 1)]
                )
        state_out.append(pltpu.make_async_copy(c_v.at[h], cc.at[:, h], co_sem.at[h]))
        state_out[h].start()
    cn_v[...] = carried_n

    def project(n):
        total = None
        for k in range(KCHUNKS):
            w_in[n][k].wait()
            span = pl.ds(k * KC, KC)
            part = jnp.dot(nb_v[:, span], w_v[n, span, :], preferred_element_type=F32)
            total = part if total is None else total + part
        return total.astype(BF16)

    queries = project(0)

    state_q = []
    for h in range(HEADS):
        qh = queries[:, DH * h : DH * (h + 1)]
        rhs = jnp.concatenate([qh, qh], axis=1)
        turned = jnp.zeros((DH, ROWS), F32)
        for b0 in range(0, SEQS, 4):
            block = c_v[h, b0 : b0 + 4].reshape(4 * DH, DH)
            out = nt_dot(jnp.concatenate(split(block), axis=1), rhs)
            for n in range(4):
                turned = jnp.where(lane[:, :ROWS] // PROPS == b0 + n, out[DH * n : DH * (n + 1)], turned)
        state_q.append(turned.T)

    for n in (8, 9, 10):
        copies[n].wait()
    gates_v[:, 0:32] = nt_dot(nb_v[...], gwt_v[...])
    for t in range(PROPS):
        gt_v[t] = gates_v[pl.ds(t, SEQS, stride=PROPS), :].T
    for h in range(HEADS):
        for g in range(2):
            shift = bias_s[g, HEADS * tp + h]
            for t in range(PROPS):
                r = 8 * h + 4 * g + t
                lane_v[r : r + 1, 0:SEQS] = gt_v[t, pl.ds(16 * g + HEADS * tp + h, 1), :] + shift
    step = lane_v[0 : 8 * HEADS, :]
    sg_v[...] = step[:, 0:SEQS]
    forget = jnp.where(igate_row, log_sigmoid(roll(step, -4, 0)), 0.0)
    cumul = cumsum4(forget, s)
    offset = step - cumul
    top = jnp.maximum(offset, jnp.where(s >= 1, roll(offset, 1, 0), NEG))
    top = jnp.maximum(top, jnp.where(s >= 2, roll(top, 2, 0), NEG))
    stable = jnp.maximum(carried_m, top)
    weight_state = jnp.exp(carried_m - stable)
    floor = jnp.exp(-(cumul + stable))
    pack = jnp.concatenate(
        [
            jnp.where(igate_row, weight_state, roll(-stable, 4, 0)),
            jnp.where(igate_row, floor, roll(offset, 4, 0)),
        ],
        axis=0,
    )
    cell = spread(pack, expand, ztile)
    ztile[0:ROWS, :] = cell
    offset_rows = ztile[...].T

    keys = project(1)
    values = project(2)
    for src, out_v in ((keys, sk_v), (values, sv_v)):
        for h in range(HEADS):
            turn_v[h] = src[:, DH * h : DH * (h + 1)].astype(F32)
            for p in range(PROPS):
                f1_v[pl.ds(h * PROPS + p, SEQS, stride=SEQS), :] = turn_v[h, pl.ds(p, SEQS, stride=PROPS), :]
        out_v[...] = f1_v[...].astype(BF16)
    outs = [(cn_v, cn), (cm_v, cm), (sk_v, sk), (sv_v, sv), (sg_v, sg), (gated_v, gated)]
    puts = [pltpu.make_async_copy(src, dst, out_sem.at[n]) for n, (src, dst) in enumerate(outs)]
    for n in range(5):
        puts[n].start()

    n_hi, n_lo = split(carried_n)
    same = (sub // PROPS == lane_full // PROPS) & (sub >= lane_full)
    same = same[:, :ROWS]
    hiddens = []
    for h in range(HEADS):
        cut = slice(DH * h, DH * (h + 1))
        qh, kh, vh = queries[:, cut], keys[:, cut], values[:, cut]
        prods = nt_dot(qh, jnp.concatenate([n_hi, n_lo, kh], axis=0))
        decay = jnp.where(
            same, cell[:, 8 * h + 4 : 8 * h + 5] + offset_rows[32 + 8 * h + 4 : 32 + 8 * h + 5, 0:ROWS], NEG
        )
        scores = prods[:, DH : DH + ROWS] * (DH ** -0.5) * jnp.exp(decay)
        carried = cell[:, 8 * h : 8 * h + 1]
        norm_q = jnp.where(lane_full % ROWS == PROPS * (sub // PROPS) + h, prods[:, :DH], 0.0)
        denom = carried * jnp.sum(norm_q, axis=-1, keepdims=True) + jnp.sum(scores, axis=-1, keepdims=True)
        numer = carried * state_q[h] + jnp.dot(
            jnp.concatenate(split(scores), axis=1), jnp.concatenate([vh, vh], axis=0), preferred_element_type=F32
        )
        hidden = numer / jnp.maximum(jnp.abs(denom), cell[:, 32 + 8 * h : 32 + 8 * h + 1])
        hidden = hidden * lax.rsqrt(jnp.mean(hidden * hidden, axis=-1, keepdims=True) + EPSILON)
        hiddens.append(hidden * hgain_v[:, cut].astype(F32))

    outgate = project(3)
    for h in range(HEADS):
        cut = slice(DH * h, DH * (h + 1))
        gated_v[:, cut] = (hiddens[h] * jax.nn.sigmoid(outgate[:, cut].astype(F32))).astype(BF16)
    puts[5].start()
    for put in puts + state_out:
        put.wait()


def front(tokens, norm_gain, wq, wk, wv, wo, gate_weight, gate_bias, head_gain, state_c, state_n, state_m,
          prev_keys, prev_values, prev_gates, accepted):
    args = (
        tokens,
        norm_gain.reshape(1, D),
        wq, wk, wv, wo,
        gate_weight.T,
        gate_bias,
        head_gain.reshape(1, MIXL),
        state_c,
        state_n.reshape(SEQS * HEADS, DH),
        state_m.T,
        prev_keys.reshape(SEQS * HEADS * PROPS, DH),
        prev_values.reshape(SEQS * HEADS * PROPS, DH),
        prev_gates.transpose(1, 2, 3, 0).reshape(HEADS * 2 * PROPS, SEQS),
        accepted.reshape(1, SEQS),
    )
    any_spec = pl.BlockSpec(memory_space=pl.ANY)
    out_shape = (
        jax.ShapeDtypeStruct((ROWS, MIXL), BF16),
        jax.ShapeDtypeStruct((SEQS, HEADS, DH, DH), F32),
        jax.ShapeDtypeStruct((SEQS * HEADS, DH), F32),
        jax.ShapeDtypeStruct((HEADS, SEQS), F32),
        jax.ShapeDtypeStruct((SEQS * HEADS * PROPS, DH), BF16),
        jax.ShapeDtypeStruct((SEQS * HEADS * PROPS, DH), BF16),
        jax.ShapeDtypeStruct((HEADS * 2 * PROPS, SEQS), F32),
    )
    vmem = pltpu.VMEM
    n_in = SEQS * HEADS * PROPS
    gated, cc, cn, cm, sk, sv, sg = pl.pallas_call(
        front_kernel,
        out_shape=out_shape,
        in_specs=[any_spec] * len(args),
        out_specs=(any_spec,) * len(out_shape),
        scratch_shapes=[
            vmem((SEQS, PROPS, D), BF16),
            vmem((1, D), BF16),
            vmem((4, D, MIXL), BF16),
            vmem((32, D), BF16),
            pltpu.SMEM((2, 16), F32),
            vmem((1, MIXL), BF16),
            vmem((HEADS, SEQS, DH, DH), F32),
            vmem((SEQS * HEADS, DH), F32),
            vmem((HEADS, SEQS), F32),
            vmem((n_in, DH), BF16),
            vmem((n_in, DH), BF16),
            vmem((32, SEQS), F32),
            vmem((1, SEQS), jnp.int32),
            vmem((ROWS, D), F32),
            vmem((ROWS, D), BF16),
            vmem((n_in, DH), F32),
            vmem((HEADS, ROWS, DH), F32),
            vmem((HEADS, ROWS, DH), F32),
            vmem((ROWS, 128), F32),
            vmem((PROPS, 128, SEQS), F32),
            vmem((48, 128), F32),
            vmem((128, 128), F32),
            vmem((ROWS, 128), F32),
            vmem((HEADS, ROWS, DH), F32),
            vmem((SEQS * HEADS, DH), F32),
            vmem((HEADS, SEQS), F32),
            vmem((n_in, DH), BF16),
            vmem((n_in, DH), BF16),
            vmem((32, SEQS), F32),
            vmem((ROWS, MIXL), BF16),
            pltpu.SemaphoreType.DMA((11,)),
            pltpu.SemaphoreType.DMA((4, KCHUNKS)),
            pltpu.SemaphoreType.DMA((HEADS,)),
            pltpu.SemaphoreType.DMA((HEADS,)),
            pltpu.SemaphoreType.DMA((6,)),
        ],
        compiler_params=pltpu.CompilerParams(vmem_limit_bytes=56 * 1024 * 1024),
        name="front",
    )(*args)
    return (
        gated,
        cc,
        cn.reshape(SEQS, HEADS, DH),
        cm.T,
        sk.reshape(SEQS, HEADS, PROPS, DH),
        sv.reshape(SEQS, HEADS, PROPS, DH),
        sg.reshape(HEADS, 2, PROPS, SEQS).transpose(3, 0, 1, 2),
    )


def joined_along(tiles, dim):
    tiles = jnp.moveaxis(tiles, 0, dim)
    lengths = tiles.shape
    return tiles.reshape(*lengths[:dim], lengths[dim] * lengths[dim + 1], *lengths[dim + 2 :])


def collect(x, axis, dim):
    peers = lax.axis_size(axis)
    got = lax.all_to_all(jnp.broadcast_to(x[None], (peers, *x.shape)), axis, 0, 0, tiled=True)
    return joined_along(got, dim)


def per_device(
    tokens, norm_gain, query_weight, key_weight, value_weight, outgate_weight, gate_weight, gate_bias, head_gain,
    out_weight, state_c, state_n, state_m, prev_keys, prev_values, prev_gates, accepted,
):
    gated, cc, cn, cm, sk, sv, sg = front(
        tokens, norm_gain, query_weight, key_weight, value_weight, outgate_weight, gate_weight, gate_bias, head_gain,
        state_c, state_n, state_m, prev_keys, prev_values, prev_gates, accepted,
    )
    partial_out = jnp.dot(collect(gated, "kv", 0), out_weight, preferred_element_type=F32)
    summed = lax.psum(partial_out, "tp")
    mixed = summed.astype(BF16).reshape(-1, PROPS, summed.shape[1])
    return (mixed, cc, cn, cm, sk, sv, sg)


IN_SPECS = (
    P("kv", None, None),
    P(),
    P(None, "tp"),
    P(None, "tp"),
    P(None, "tp"),
    P(None, "tp"),
    P(),
    P(),
    P("tp"),
    P("tp", "kv"),
    P("kv", "tp", None, None),
    P("kv", "tp", None),
    P("kv", "tp"),
    P("kv", "tp", None, None),
    P("kv", "tp", None, None),
    P("kv", "tp", None, None),
    P("kv"),
)
OUT_SPECS = (
    P(None, None, "kv"),
    P("kv", "tp", None, None),
    P("kv", "tp", None),
    P("kv", "tp"),
    P("kv", "tp", None, None),
    P("kv", "tp", None, None),
    P("kv", "tp", None, None),
)


def solution(mesh):
    return jax.shard_map(per_device, mesh=mesh, in_specs=IN_SPECS, out_specs=OUT_SPECS, check_vma=False)
```

```python
import functools

import jax
import jax.numpy as jnp
from jax import lax
from jax.experimental import pallas as pl
from jax.experimental.pallas import tpu as pltpu
from jax.sharding import PartitionSpec as P

EPSILON = 1e-06
NEG = -1e30
F32 = jnp.float32
BF16 = jnp.bfloat16
NT = (((1,), (1,)), ((), ()))

SEQS = 16
PROPS = 4
HEADS = 4
DH = 128
D = 4096
ROWS = SEQS * PROPS
MIXL = HEADS * DH
KCHUNKS = 4
KC = D // KCHUNKS


def nt_dot(a, b):
    return lax.dot_general(a, b, NT, preferred_element_type=F32)


def split(x):
    hi = x.astype(BF16)
    return hi, (x - hi.astype(F32)).astype(BF16)


def log_sigmoid(x):
    return jnp.minimum(x, 0.0) - jnp.log1p(jnp.exp(-jnp.abs(x)))


def roll(x, shift, axis):
    return pltpu.roll(x, shift % x.shape[axis], axis)


def iota(shape, axis):
    return lax.broadcasted_iota(jnp.int32, shape, axis)


def cumsum4(x, s):
    x = x + jnp.where(s >= 1, roll(x, 1, 0), 0.0)
    return x + jnp.where(s >= 2, roll(x, 2, 0), 0.0)


def spread(packed, expand, ztile):
    rows = packed.shape[0]
    ztile[0:rows, :] = packed
    turned = ztile[...].T
    for s in range(PROPS):
        expand[pl.ds(s, SEQS, stride=PROPS), :] = turned[0:SEQS, :]
    wide = expand[...]
    own = jnp.where(iota(wide.shape, 1) % PROPS == iota(wide.shape, 0) % PROPS, wide, 0.0)
    return own + roll(own, -1, 1) + roll(own, -2, 1) + roll(own, -3, 1)


def front_kernel(
    tok, gain, wq, wk, wv, wo, gwt, bias, hgain, sc, sn, sm, pk, pv, pg, acc,
    gated, cc, cn, cm, sk, sv, sg,
    tok_v, gain_v, w_v, gwt_v, bias_s, hgain_v, c_v, sn_v, sm_v, pk_v, pv_v, pg_v, acc_v,
    x_v, nb_v, f1_v, kp_v, vp_v, gates_v, gt_v, lane_v, ztile, expand, turn_v, cn_v, cm_v, sk_v, sv_v, sg_v, gated_v,
    in_sem, w_sem, c_sem, co_sem, out_sem,
):
    tp = lax.axis_index("tp")
    small = [
        (pg, pg_v), (acc, acc_v), (sm, sm_v), (pk, pk_v), (pv, pv_v), (tok, tok_v), (gain, gain_v),
        (sn, sn_v), (bias, bias_s), (hgain, hgain_v), (gwt, gwt_v),
    ]
    copies = {}
    for n, (src, dst) in enumerate(small):
        copies[n] = pltpu.make_async_copy(src, dst, in_sem.at[n])
        copies[n].start()
    state_in = []
    for h in range(HEADS):
        state_in.append(pltpu.make_async_copy(sc.at[:, h], c_v.at[h], c_sem.at[h]))
        state_in[h].start()
    w_in = []
    for n, w in enumerate((wq, wk, wv, wo)):
        w_in.append([])
        for k in range(KCHUNKS):
            span = pl.ds(k * KC, KC)
            w_in[n].append(pltpu.make_async_copy(w.at[span], w_v.at[n, span], w_sem.at[n, k]))
            w_in[n][k].start()

    row = iota((8 * HEADS, 128), 0)
    s = row % PROPS
    igate_row = row % 8 < PROPS
    lane_v[...] = jnp.zeros_like(lane_v)
    ztile[...] = jnp.zeros_like(ztile)

    for n in range(3):
        copies[n].wait()
    lane_v[0 : 8 * HEADS, 0:SEQS] = pg_v[...]
    lane_v[32:33, 0:SEQS] = acc_v[...].astype(F32)
    lane_v[40:44, 0:SEQS] = sm_v[...]
    igates = lane_v[0 : 8 * HEADS, :]
    accepted = lane_v[32:33, :]
    state_m = jnp.concatenate(
        [jnp.broadcast_to(lane_v[40 + h : 41 + h, :], (8, 128)) for h in range(HEADS)], axis=0
    )
    within = (s.astype(F32) < accepted) & igate_row
    masked = jnp.where(within, log_sigmoid(roll(igates, -4, 0)), 0.0)
    cums = cumsum4(masked, s)
    summed = jnp.where((s == 3) & igate_row, cums, 0.0)
    summed = summed + roll(summed, -1, 0)
    summed = summed + roll(summed, -2, 0)
    log_weight = jnp.where(within, summed - cums + igates, NEG)
    top = jnp.maximum(log_weight, jnp.where(s % 2 == 0, roll(log_weight, -1, 0), roll(log_weight, 1, 0)))
    top = jnp.maximum(top, jnp.where(s < 2, roll(top, -2, 0), roll(top, 2, 0)))
    carried_m = jnp.maximum(summed + state_m, top)
    shrink = jnp.exp(summed + state_m - carried_m)
    weights = jnp.exp(log_weight - carried_m)
    for h in range(HEADS):
        cm_v[h : h + 1, :] = carried_m[8 * h : 8 * h + 1, 0:SEQS]
    cols = spread(jnp.where(igate_row, weights, roll(shrink, 4, 0)), expand, ztile)

    copies[3].wait()
    copies[4].wait()
    for src, dst in ((pk_v, kp_v), (pv_v, vp_v)):
        f1_v[...] = src[...].astype(F32)
        for h in range(HEADS):
            for p in range(PROPS):
                dst[h, pl.ds(p, SEQS, stride=PROPS), :] = f1_v[pl.ds(h * PROPS + p, SEQS, stride=SEQS), :]

    copies[5].wait()
    copies[6].wait()
    for b in range(SEQS):
        x_v[PROPS * b : PROPS * (b + 1), :] = tok_v[b].astype(F32)
    gain_f = gain_v[...].astype(F32)
    for r in range(0, ROWS, 16):
        x = x_v[r : r + 16, :]
        scale = lax.rsqrt(jnp.mean(x * x, axis=-1, keepdims=True) + EPSILON)
        for c in range(D // 128):
            cut = slice(128 * c, 128 * (c + 1))
            nb_v[r : r + 16, cut] = (x[:, cut] * scale * gain_f[c : c + 1, :]).astype(BF16)

    copies[7].wait()
    lane = iota((1, 128), 1)
    sub = iota((ROWS, 128), 0)
    lane_full = iota((ROWS, 128), 1)
    shrink_bh = jnp.sum(
        jnp.where(lane_full == 8 * (sub % HEADS) + 4, cols, 0.0), axis=-1, keepdims=True
    )
    carried_n = shrink_bh * sn_v[...]
    state_out = []
    for h in range(HEADS):
        wkeys = kp_v[h] * (DH ** -0.5) * cols[:, 8 * h : 8 * h + 1]
        total = wkeys + jnp.where(sub % 2 == 0, roll(wkeys, -1, 0), roll(wkeys, 1, 0))
        total = total + jnp.where(sub % 4 < 2, roll(total, -2, 0), roll(total, 2, 0))
        carried_n = carried_n + jnp.where(sub % HEADS == h, total, 0.0)
        rhs = jnp.concatenate(split(wkeys), axis=0)
        vp = vp_v[h]
        vt = jnp.concatenate([vp, vp], axis=0).T.astype(BF16)
        state_in[h].wait()
        for b0 in range(0, SEQS, 4):
            lhs = jnp.concatenate(
                [vt * ((lane % ROWS) // PROPS == b).astype(F32).astype(BF16) for b in range(b0, b0 + 4)], axis=0
            )
            update = jnp.dot(lhs, rhs, preferred_element_type=F32)
            for n in range(4):
                b = b0 + n
                c_v[h, b] = (
                    cols[PROPS * b : PROPS * b + 1, 8 * h + 4 : 8 * h + 5] * c_v[h, b]
                    + update[DH * n : DH * (n + 1)]
                )
        state_out.append(pltpu.make_async_copy(c_v.at[h], cc.at[:, h], co_sem.at[h]))
        state_out[h].start()
    cn_v[...] = carried_n

    def project(n):
        total = None
        for k in range(KCHUNKS):
            w_in[n][k].wait()
            span = pl.ds(k * KC, KC)
            part = jnp.dot(nb_v[:, span], w_v[n, span, :], preferred_element_type=F32)
            total = part if total is None else total + part
        return total.astype(BF16)

    queries = project(0)

    state_q = []
    for h in range(HEADS):
        qh = queries[:, DH * h : DH * (h + 1)]
        rhs = jnp.concatenate([qh, qh], axis=1)
        turned = jnp.zeros((DH, ROWS), F32)
        for b0 in range(0, SEQS, 4):
            block = c_v[h, b0 : b0 + 4].reshape(4 * DH, DH)
            out = nt_dot(jnp.concatenate(split(block), axis=1), rhs)
            for n in range(4):
                turned = jnp.where(lane[:, :ROWS] // PROPS == b0 + n, out[DH * n : DH * (n + 1)], turned)
        state_q.append(turned.T)

    for n in (8, 9, 10):
        copies[n].wait()
    gates_v[:, 0:32] = nt_dot(nb_v[...], gwt_v[...])
    for t in range(PROPS):
        gt_v[t] = gates_v[pl.ds(t, SEQS, stride=PROPS), :].T
    for h in range(HEADS):
        for g in range(2):
            shift = bias_s[g, HEADS * tp + h]
            for t in range(PROPS):
                r = 8 * h + 4 * g + t
                lane_v[r : r + 1, 0:SEQS] = gt_v[t, pl.ds(16 * g + HEADS * tp + h, 1), :] + shift
    step = lane_v[0 : 8 * HEADS, :]
    sg_v[...] = step[:, 0:SEQS]
    forget = jnp.where(igate_row, log_sigmoid(roll(step, -4, 0)), 0.0)
    cumul = cumsum4(forget, s)
    offset = step - cumul
    top = jnp.maximum(offset, jnp.where(s >= 1, roll(offset, 1, 0), NEG))
    top = jnp.maximum(top, jnp.where(s >= 2, roll(top, 2, 0), NEG))
    stable = jnp.maximum(carried_m, top)
    weight_state = jnp.exp(carried_m - stable)
    floor = jnp.exp(-(cumul + stable))
    pack = jnp.concatenate(
        [
            jnp.where(igate_row, weight_state, roll(-stable, 4, 0)),
            jnp.where(igate_row, floor, roll(offset, 4, 0)),
        ],
        axis=0,
    )
    cell = spread(pack, expand, ztile)
    ztile[0:ROWS, :] = cell
    offset_rows = ztile[...].T

    keys = project(1)
    values = project(2)
    for src, out_v in ((keys, sk_v), (values, sv_v)):
        for h in range(HEADS):
            turn_v[h] = src[:, DH * h : DH * (h + 1)].astype(F32)
            for p in range(PROPS):
                f1_v[pl.ds(h * PROPS + p, SEQS, stride=SEQS), :] = turn_v[h, pl.ds(p, SEQS, stride=PROPS), :]
        out_v[...] = f1_v[...].astype(BF16)
    outs = [(cn_v, cn), (cm_v, cm), (sk_v, sk), (sv_v, sv), (sg_v, sg), (gated_v, gated)]
    puts = [pltpu.make_async_copy(src, dst, out_sem.at[n]) for n, (src, dst) in enumerate(outs)]
    for n in range(5):
        puts[n].start()

    n_hi, n_lo = split(carried_n)
    same = (sub // PROPS == lane_full // PROPS) & (sub >= lane_full)
    same = same[:, :ROWS]
    hiddens = []
    for h in range(HEADS):
        cut = slice(DH * h, DH * (h + 1))
        qh, kh, vh = queries[:, cut], keys[:, cut], values[:, cut]
        prods = nt_dot(qh, jnp.concatenate([n_hi, n_lo, kh], axis=0))
        decay = jnp.where(
            same, cell[:, 8 * h + 4 : 8 * h + 5] + offset_rows[32 + 8 * h + 4 : 32 + 8 * h + 5, 0:ROWS], NEG
        )
        scores = prods[:, DH : DH + ROWS] * (DH ** -0.5) * jnp.exp(decay)
        carried = cell[:, 8 * h : 8 * h + 1]
        norm_q = jnp.where(lane_full % ROWS == PROPS * (sub // PROPS) + h, prods[:, :DH], 0.0)
        denom = carried * jnp.sum(norm_q, axis=-1, keepdims=True) + jnp.sum(scores, axis=-1, keepdims=True)
        numer = carried * state_q[h] + jnp.dot(
            jnp.concatenate(split(scores), axis=1), jnp.concatenate([vh, vh], axis=0), preferred_element_type=F32
        )
        hidden = numer / jnp.maximum(jnp.abs(denom), cell[:, 32 + 8 * h : 32 + 8 * h + 1])
        hidden = hidden * lax.rsqrt(jnp.mean(hidden * hidden, axis=-1, keepdims=True) + EPSILON)
        hiddens.append(hidden * hgain_v[...].astype(F32)[h : h + 1])

    outgate = project(3)
    for h in range(HEADS):
        cut = slice(DH * h, DH * (h + 1))
        gated_v[:, cut] = (hiddens[h] * jax.nn.sigmoid(outgate[:, cut].astype(F32))).astype(BF16)
    puts[5].start()
    for put in puts + state_out:
        put.wait()


def front(tokens, norm_gain, wq, wk, wv, wo, gate_weight, gate_bias, head_gain, state_c, state_n, state_m,
          prev_keys, prev_values, prev_gates, accepted):
    args = (
        tokens,
        norm_gain.reshape(D // 128, 128),
        wq, wk, wv, wo,
        gate_weight.T,
        gate_bias,
        head_gain.reshape(HEADS, DH),
        state_c,
        state_n.reshape(SEQS * HEADS, DH),
        state_m.T,
        prev_keys.reshape(SEQS * HEADS * PROPS, DH),
        prev_values.reshape(SEQS * HEADS * PROPS, DH),
        prev_gates.transpose(1, 2, 3, 0).reshape(HEADS * 2 * PROPS, SEQS),
        accepted.reshape(1, SEQS),
    )
    any_spec = pl.BlockSpec(memory_space=pl.ANY)
    out_shape = (
        jax.ShapeDtypeStruct((ROWS, MIXL), BF16),
        jax.ShapeDtypeStruct((SEQS, HEADS, DH, DH), F32),
        jax.ShapeDtypeStruct((SEQS * HEADS, DH), F32),
        jax.ShapeDtypeStruct((HEADS, SEQS), F32),
        jax.ShapeDtypeStruct((SEQS * HEADS * PROPS, DH), BF16),
        jax.ShapeDtypeStruct((SEQS * HEADS * PROPS, DH), BF16),
        jax.ShapeDtypeStruct((HEADS * 2 * PROPS, SEQS), F32),
    )
    vmem = pltpu.VMEM
    n_in = SEQS * HEADS * PROPS
    gated, cc, cn, cm, sk, sv, sg = pl.pallas_call(
        front_kernel,
        out_shape=out_shape,
        in_specs=[any_spec] * len(args),
        out_specs=(any_spec,) * len(out_shape),
        scratch_shapes=[
            vmem((SEQS, PROPS, D), BF16),
            vmem((D // 128, 128), BF16),
            vmem((4, D, MIXL), BF16),
            vmem((32, D), BF16),
            pltpu.SMEM((2, 16), F32),
            vmem((HEADS, DH), BF16),
            vmem((HEADS, SEQS, DH, DH), F32),
            vmem((SEQS * HEADS, DH), F32),
            vmem((HEADS, SEQS), F32),
            vmem((n_in, DH), BF16),
            vmem((n_in, DH), BF16),
            vmem((32, SEQS), F32),
            vmem((1, SEQS), jnp.int32),
            vmem((ROWS, D), F32),
            vmem((ROWS, D), BF16),
            vmem((n_in, DH), F32),
            vmem((HEADS, ROWS, DH), F32),
            vmem((HEADS, ROWS, DH), F32),
            vmem((ROWS, 128), F32),
            vmem((PROPS, 128, SEQS), F32),
            vmem((48, 128), F32),
            vmem((128, 128), F32),
            vmem((ROWS, 128), F32),
            vmem((HEADS, ROWS, DH), F32),
            vmem((SEQS * HEADS, DH), F32),
            vmem((HEADS, SEQS), F32),
            vmem((n_in, DH), BF16),
            vmem((n_in, DH), BF16),
            vmem((32, SEQS), F32),
            vmem((ROWS, MIXL), BF16),
            pltpu.SemaphoreType.DMA((11,)),
            pltpu.SemaphoreType.DMA((4, KCHUNKS)),
            pltpu.SemaphoreType.DMA((HEADS,)),
            pltpu.SemaphoreType.DMA((HEADS,)),
            pltpu.SemaphoreType.DMA((6,)),
        ],
        compiler_params=pltpu.CompilerParams(vmem_limit_bytes=56 * 1024 * 1024),
        name="front",
    )(*args)
    return (
        gated,
        cc,
        cn.reshape(SEQS, HEADS, DH),
        cm.T,
        sk.reshape(SEQS, HEADS, PROPS, DH),
        sv.reshape(SEQS, HEADS, PROPS, DH),
        sg.reshape(HEADS, 2, PROPS, SEQS).transpose(3, 0, 1, 2),
    )


MESH = pl.DeviceIdType.MESH
SIDE = 4
CORES = 2
GROUPS = (
    ((0, 0), (1, 0), (3, 0), (0, 1), (0, 3)),
    ((1, 1), (1, 3), (3, 1), (3, 3), (2, 0), (0, 2)),
    ((2, 1), (2, 3), (1, 2), (3, 2), (2, 2)),
)
RB = ROWS // SIDE
FIRST = (1, 3, 2)
SPREAD = (0, 1, 3, 2)
MIX = MIXL * SIDE


def exchange_kernel(
    gated, weight, out,
    g_v, w_v, o_v, r_v,
    loc_sem, a_send, a_recv, w_send, w_recv, f_send, f_recv, s_send, s_recv, r_send, r_recv, c_send, c_recv, o_sem,
):
    kv, x = lax.axis_index("kv"), lax.axis_index("tp")
    z, y, core = kv // (SIDE * CORES), kv // CORES % SIDE, kv % CORES
    other = 1 - core

    def at(dz=0, dy=0, same=True, dx=0):
        zz, yy, xx = (z + dz) % SIDE, (y + dy) % SIDE, (x + dx) % SIDE
        return ((zz * SIDE + yy) * CORES + (core if same else other), xx)

    def place(dz, dy):
        return (z + dz) % SIDE * SIDE + (y + dy) % SIDE

    def wcols(c):
        return pl.ds(pl.multiple_of(c * DH, DH), DH)

    def kcols(xx):
        return pl.ds(pl.multiple_of(xx * MIXL, MIXL), MIXL)

    partners = [at(dx=d) for d in (1, 2, 3)] + [at(same=False, dx=d) for d in range(4)]
    partners += [at(dy=d) for d in (1, 2, 3)] + [at(dz=d) for d in (1, 2, 3)]
    own_w = w_v.at[kcols(x), wcols(core)]
    load_w = pltpu.make_async_copy(weight, own_w, loc_sem.at[0])
    load_w.start()
    barrier = pltpu.get_barrier_semaphore()
    for device in partners:
        pl.semaphore_signal(barrier, inc=1, device_id=device, device_id_type=MESH)
    pl.semaphore_wait(barrier, len(partners))

    sends = []

    def send(src, dst, ssem, rsem, device):
        copy = pltpu.make_async_remote_copy(
            src_ref=src, dst_ref=dst, send_sem=ssem, recv_sem=rsem, device_id=device, device_id_type=MESH
        )
        copy.start()
        sends.append(copy)

    def arrived(dst, ssem, rsem):
        pltpu.make_async_remote_copy(
            src_ref=dst, dst_ref=dst, send_sem=ssem, recv_sem=rsem, device_id=at(dx=1), device_id_type=MESH
        ).wait_recv()

    mine = place(0, 0)
    for d in (1, 3, 2):
        rows = pl.ds(pl.multiple_of((x + d) % SIDE * RB, RB), RB)
        send(gated.at[rows], g_v.at[mine, :, kcols(x)], a_send.at[d - 1], a_recv.at[d - 1], at(dx=d))
    keep = pltpu.make_async_copy(
        gated.at[pl.ds(pl.multiple_of(x * RB, RB), RB)], g_v.at[mine, :, kcols(x)], loc_sem.at[1]
    )
    keep.start()

    load_w.wait()
    for d in (1, 3, 2):
        send(own_w, own_w, w_send.at[d], w_recv.at[0, d], at(dx=d))
    send(own_w, own_w, w_send.at[0], w_recv.at[1, 0], at(same=False))

    def pass_weight(d):
        piece = w_v.at[kcols((x - d) % SIDE), wcols(core)]
        arrived(piece, w_send.at[d], w_recv.at[0, d])
        send(piece, piece, w_send.at[3 + d], w_recv.at[1, d], at(same=False))

    keep.wait()
    for d in (1, 3, 2):
        arrived(g_v.at[mine, :, kcols((x - d) % SIDE)], a_send.at[d - 1], a_recv.at[d - 1])

    def offsets(half, first, second):
        return (second, first) if half == 0 else (first, second)

    def block(half, first, second, part=None):
        columns = MIX // 2
        start = half * columns
        if part is not None:
            columns //= 2
            start += part * columns
        return g_v.at[place(*offsets(half, first, second)), :, pl.ds(start, columns)]

    def to(half, first, second):
        return at(*offsets(half, first, second))

    def send_first(half):
        for n, d in enumerate(FIRST):
            send(block(half, 0, 0), block(half, 0, 0), f_send.at[half, n], f_recv.at[half, n], to(half, d, 0))

    def send_spread(half, n):
        for k, hop in enumerate((1, 3)):
            piece = block(half, SPREAD[n], 0)
            send(piece, piece, s_send.at[half, n, k], s_recv.at[half, n, k], to(half, 0, hop))

    def wait_first(half, n):
        arrived(block(half, SIDE - FIRST[n], 0), f_send.at[half, n], f_recv.at[half, n])

    def wait_spread(half, n, k):
        hop = (1, 3)[k]
        arrived(block(half, SPREAD[n], SIDE - hop), s_send.at[half, n, k], s_recv.at[half, n, k])

    def relay(half, n, k):
        hop = (1, 3)[k]
        wait_spread(half, n, k)
        piece = block(half, SPREAD[n], SIDE - hop, k)
        send(piece, piece, r_send.at[half, n, k], r_recv.at[half, n, k], to(half, 0, hop))

    def wait_relay(half, n):
        for k in range(2):
            arrived(block(half, SPREAD[n], 2, k), r_send.at[half, n, k], r_recv.at[half, n, k])

    places = [place(*offset) for group in GROUPS for offset in group]
    starts = [0]
    for group in GROUPS:
        starts.append(starts[-1] + len(group))

    def c_sends(n):
        span = pl.ds(starts[n], starts[n + 1] - starts[n])
        target = o_v.at[span, core, x]
        for d in (1, 3, 2):
            send(target, target, c_send.at[n, 0, d], c_recv.at[n, 0, d], at(dx=d))
            send(r_v.at[span], target, c_send.at[n, 1, d], c_recv.at[n, 1, d], at(same=False, dx=d))
        send(r_v.at[span], target, c_send.at[n, 1, 0], c_recv.at[n, 1, 0], at(same=False))

    def multiply(n):
        lhs = jnp.concatenate([g_v[places[r]] for r in range(starts[n], starts[n + 1])], axis=0)
        result = jnp.dot(lhs, w_v[...], preferred_element_type=F32).astype(BF16)
        low, high = result[:, :DH], result[:, DH:]
        here = jnp.where(core == 0, low, high)
        there = jnp.where(core == 0, high, low)
        for i, r in enumerate(range(starts[n], starts[n + 1])):
            o_v[r, core, x] = here[RB * i : RB * (i + 1)]
            r_v[r] = there[RB * i : RB * (i + 1)]
        c_sends(n)

    for half in range(2):
        send_first(half)
        send_spread(half, 0)
    for half in range(2):
        for n in (0, 1):
            wait_first(half, n)
            send_spread(half, SPREAD.index(SIDE - FIRST[n]))
    for half in range(2):
        for k in range(2):
            relay(half, 0, k)
    for half in range(2):
        wait_first(half, 2)
        send_spread(half, 3)
    for d in (1, 3, 2):
        pass_weight(d)
    for n in (1, 2):
        for half in range(2):
            for k in range(2):
                relay(half, n, k)
    for d in range(SIDE):
        arrived(w_v.at[kcols((x - d) % SIDE), wcols(other)], w_send.at[d], w_recv.at[1, d])
    multiply(0)
    for half in range(2):
        for k in range(2):
            relay(half, 3, k)
    for half in range(2):
        wait_relay(half, 0)
    multiply(1)
    for n in (1, 2, 3):
        for half in range(2):
            wait_relay(half, n)
    multiply(2)

    puts = []
    for n in range(len(GROUPS)):
        span = pl.ds(starts[n], starts[n + 1] - starts[n])
        for d in range(SIDE):
            xx = (x - d) % SIDE
            if d:
                arrived(o_v.at[span, core, xx], c_send.at[n, 0, d], c_recv.at[n, 0, d])
            arrived(o_v.at[span, other, xx], c_send.at[n, 1, d], c_recv.at[n, 1, d])
        for r in range(starts[n], starts[n + 1]):
            puts.append(pltpu.make_async_copy(o_v.at[r], out.at[places[r]], o_sem.at[r]))
            puts[-1].start()
    for copy in sends:
        copy.wait_send()
    for put in puts:
        put.wait()


def exchange(gated, weight):
    dma = pltpu.SemaphoreType.DMA
    blocks = SIDE * SIDE
    out = pl.pallas_call(
        exchange_kernel,
        out_shape=jax.ShapeDtypeStruct((blocks, CORES, SIDE, RB, DH), BF16),
        in_specs=[pl.BlockSpec(memory_space=pltpu.VMEM), pl.BlockSpec(memory_space=pl.ANY)],
        out_specs=pl.BlockSpec(memory_space=pl.ANY),
        scratch_shapes=[
            pltpu.VMEM((blocks, RB, MIX), BF16),
            pltpu.VMEM((MIX, CORES * DH), BF16),
            pltpu.VMEM((blocks, CORES, SIDE, RB, DH), BF16),
            pltpu.VMEM((blocks, RB, DH), BF16),
            dma((2,)),
            dma((3,)), dma((3,)),
            dma((7,)), dma((2, 4)),
            dma((2, 3)), dma((2, 3)),
            dma((2, 4, 2)), dma((2, 4, 2)),
            dma((2, 4, 2)), dma((2, 4, 2)),
            dma((3, 2, 4)), dma((3, 2, 4)),
            dma((blocks,)),
        ],
        compiler_params=pltpu.CompilerParams(
            collective_id=0, has_side_effects=True, vmem_limit_bytes=32 * 1024 * 1024
        ),
        name="exchange",
    )(gated, weight)
    return out.reshape(SEQS * CORES * blocks, PROPS, DH)


def per_device(
    tokens, norm_gain, query_weight, key_weight, value_weight, outgate_weight, gate_weight, gate_bias, head_gain,
    out_weight, state_c, state_n, state_m, prev_keys, prev_values, prev_gates, accepted,
):
    gated, cc, cn, cm, sk, sv, sg = front(
        tokens, norm_gain, query_weight, key_weight, value_weight, outgate_weight, gate_weight, gate_bias, head_gain,
        state_c, state_n, state_m, prev_keys, prev_values, prev_gates, accepted,
    )
    mixed = exchange(gated, out_weight)
    return (mixed, cc, cn, cm, sk, sv, sg)


IN_SPECS = (
    P("kv", None, None),
    P(),
    P(None, "tp"),
    P(None, "tp"),
    P(None, "tp"),
    P(None, "tp"),
    P(),
    P(),
    P("tp"),
    P("tp", "kv"),
    P("kv", "tp", None, None),
    P("kv", "tp", None),
    P("kv", "tp"),
    P("kv", "tp", None, None),
    P("kv", "tp", None, None),
    P("kv", "tp", None, None),
    P("kv"),
)
OUT_SPECS = (
    P(None, None, "kv"),
    P("kv", "tp", None, None),
    P("kv", "tp", None),
    P("kv", "tp"),
    P("kv", "tp", None, None),
    P("kv", "tp", None, None),
    P("kv", "tp", None, None),
)


def solution(mesh):
    return jax.shard_map(per_device, mesh=mesh, in_specs=IN_SPECS, out_specs=OUT_SPECS, check_vma=False)
```
